32 devices in a mesh: ep: 8 (over z, y), tp: 4 (over x, core).
Axes of the slice: x: 2, y: 2, z: 4, core: 2. Of those that a mesh axis runs over, the one named last changes fastest.
Arguments:
- mixer_microbatch: bfloat16 [8192, 2048], P(('ep', 'tp')), may hold values from -6 to 6
- mixer_gain_vector: float32 [2048], replicated, may hold values from 0.1 to 1.9
- asker_matrix: bfloat16 [2048, 1024], P(None, 'tp'), may hold values from -0.125 to 0.125
- matcher_matrix: bfloat16 [2048, 1024], P(None, 'tp'), may hold values from -0.125 to 0.125
- fading_matrix: bfloat16 [2048, 1024], P(None, 'tp'), may hold values from -0.125 to 0.125
- content_matrix: bfloat16 [2048, 2048], P(None, 'tp'), may hold values from -0.125 to 0.125
- result_valve_matrix: bfloat16 [2048, 2048], P(None, 'tp'), may hold values from -0.125 to 0.125
- fading_shift_vector: float32 [1024], P('tp'), may hold values from -1.5 to 20
- extra_fade_amount: float32 [8192, 16], P('ep', 'tp'), may hold values from -0.7 to 0
- starting_memory: float32 [1024, 128], P('tp'), may hold values from -24 to 24
- subspace_gain_vector: float32 [2048], P('tp'), may hold values from 0.1 to 1.9
- result_matrix: bfloat16 [2048, 2048], replicated, may hold values from -0.125 to 0.125
- specialist_microbatch: bfloat16 [4096, 2048], P(('ep', 'tp')), may hold values from -6 to 6
- specialist_gain_vector: float32 [2048], replicated, may hold values from 0.1 to 1.9
- picked_specialists: int32 [4096, 2], P(('ep', 'tp')), may hold values from 0 to 15, all different within a row; in each aligned block of 128 rows (0 to 127, 128 to 255, ...) at most 24 rows name the same one
- specialist_mixing_factor: float32 [4096, 2], P(('ep', 'tp')), may hold values from 0.3 to 1.5
- specialist_valve_matrix: bfloat16 [16, 2048, 1024], P('ep', None, 'tp'), may hold values from -0.125 to 0.125
- specialist_widen_matrix: bfloat16 [16, 2048, 1024], P('ep', None, 'tp'), may hold values from -0.125 to 0.125
- specialist_shrink_matrix: bfloat16 [16, 1024, 2048], P('ep', 'tp'), may hold values from -0.1875 to 0.1875
- joint_valve_matrix: bfloat16 [2048, 512], P(None, 'tp'), may hold values from -0.125 to 0.125
- joint_widen_matrix: bfloat16 [2048, 512], P(None, 'tp'), may hold values from -0.125 to 0.125
- joint_shrink_matrix: bfloat16 [512, 2048], P('tp'), may hold values from -0.25 to 0.25
Outputs:
- mixer_sublayer_result: bfloat16 [8192, 2048], P(('ep', 'tp'))
- moe_out: bfloat16 [4096, 2048], P(('ep', 'tp'))
The draws below stay inside these ranges and needn't reach their ends.
Inputs may be any that keep to these rules, and one draw needn't show every extreme that they name: `picked_specialists`: each row names 2 different experts; among the rows of one device no expert is named more than 24 times.
All inputs are finite; a program needn't handle non-finite values.
Results may differ from the reference program's by a relative error of at most 0.025.
Values may be sent and summed in bfloat16 or wider, within the bound.
A program may use at most 192 MiB of HBM per device.

```python
import math
import jax
import jax.numpy as jnp
import numpy as np
from jax import lax

D = 2048
NUM_SUBSPACES = 16
MATCHER_WIDTH = 64
DV = 128
SPAN_LENGTH = 64
TOK_MOE = 128
TOP_K = 2
FFE = 1024
FFS = 512
EXPERTS = 16
CAP = 24
TOKENS_A = 8192
TOKENS_B = 4096
N_EP = 8
N_TP = 4


def draw_fading_shift_vector(key, part):
    key_one, key_two, key_three = jax.random.split(jax.random.fold_in(key, 11), 3)
    shuffled = jax.random.permutation(key_one, NUM_SUBSPACES)
    fast_head = shuffled < NUM_SUBSPACES // 2
    slow_value = jnp.log(jnp.float32(TOKENS_A) * 0.206)
    fast_value = jax.random.uniform(key_two, (NUM_SUBSPACES, MATCHER_WIDTH), jnp.float32, -1.0, 0.5)
    jitter = jax.random.uniform(key_three, (NUM_SUBSPACES, MATCHER_WIDTH), jnp.float32, -0.5, 0.5)
    result_value = jnp.where(fast_head[:, None], fast_value, slow_value + jitter)
    return result_value.reshape(NUM_SUBSPACES * MATCHER_WIDTH).astype(jnp.float32)


def draw_extra_fade_amount(key, part):
    key_one, key_two = jax.random.split(jax.random.fold_in(key, 23), 2)
    where_rows = jax.random.randint(key_one, (3,), 0, TOKENS_A)
    drop_depth = jnp.log(jax.random.uniform(key_two, (3, NUM_SUBSPACES), jnp.float32, 0.5, 0.8))
    positions = jnp.arange(TOKENS_A, dtype=jnp.int32)
    matches = (positions[:, None] == where_rows[None, :]).astype(jnp.float32)
    return jnp.dot(matches, drop_depth, precision=lax.Precision.HIGHEST)


def block_scale(rng, extent, cuts, least, largest):
    factor_of = 1.0
    for axis_at, parts in cuts:
        steps = jax.random.uniform(jax.random.fold_in(jax.random.fold_in(rng, 6), axis_at), (parts,), jnp.float32, least / len(cuts), largest / len(cuts))
        factor_of = factor_of * jnp.repeat(jnp.exp(steps), extent[axis_at] // parts).reshape((-1,) + (1,) * (len(extent) - 1 - axis_at))
    return factor_of


def shared_out(key, own, number, rows, amount, top, limit, slope):
    ranking = jax.random.permutation(key, amount)
    packed, ordinary = portions_of(amount, rows * top, limit, slope, True), portions_of(amount, rows * top, limit, slope, False)
    places = jnp.arange(amount)

    def named(sizes, offset_by):
        used = int((sizes > 0).sum())
        fixed = max(1, used // 4)
        moved = fixed + (places - fixed + offset_by * (used - fixed)) % max(1, amount - fixed)
        return jnp.zeros((amount,), jnp.int32).at[ranking[jnp.where(places < fixed, places, moved)]].set(jnp.asarray(sizes, jnp.int32))

    sizes = jnp.where(number % 4 == 0, named(packed, number // 4), named(ordinary, number - number // 4 - 1))
    mixed = jax.random.permutation(jax.random.fold_in(own, 3), amount)
    giver, receiver = mixed[0:amount // 2 * 2:2], mixed[1:amount // 2 * 2:2]
    margin = jnp.minimum(sizes[giver] - 1, limit - sizes[receiver]) // 2
    margin = jnp.where((giver == ranking[0]) | (receiver == ranking[0]) | (sizes[receiver] == 0), 0, jnp.maximum(margin, 0))
    moved = jax.random.randint(jax.random.fold_in(own, 4), (amount // 2,), 0, 1 << 20) % (margin + 1)
    sizes = sizes.at[giver].add(-moved).at[receiver].add(moved)
    members = jnp.searchsorted(jnp.cumsum(sizes), jnp.arange(rows * top), side="right").astype(jnp.int32)
    listing = members.reshape(top, rows).T
    listing = listing[jax.random.permutation(jax.random.fold_in(own, 1), rows)]
    offset_by = jax.random.randint(jax.random.fold_in(own, 2), (rows, 1), 0, top)
    return jnp.take_along_axis(listing, (jnp.arange(top)[None, :] + offset_by) % top, axis=1)


def portions_of(number_of, total, most, lean, full):
    portions = [(1 << 20) // math.isqrt(grade ** lean) + 1 for grade in range(1, number_of + 1)]
    largest = most if full else min(most, max(-(-total // number_of), total * portions[0] // sum(portions)))
    least = 1 if total - largest >= number_of - 1 else 0
    holding, spare = [largest] + [least] * (number_of - 1), total - largest - least * (number_of - 1)
    while spare > 0:
        free = [i for i in range(1, number_of) if holding[i] < largest] or [i for i in range(1, number_of) if holding[i] < most]
        mass, left = sum([portions[i] for i in free]), spare
        for i in free:
            more = min(most - holding[i], max(1, left * portions[i] // mass), spare)
            holding[i] = holding[i] + more
            spare = spare - more
    return np.array(holding)


def bell_draw(rng, dims, scale, limit, cuts=(), held_as=jnp.bfloat16):
    drawn = jax.random.normal(rng, dims, jnp.float32) * scale
    if len(cuts) > 0:
        drawn = block_scale(rng, dims, cuts, -0.22, 0.18) * drawn
    return jnp.clip(drawn, min=-limit, max=limit).astype(held_as)


def setup_inputs(seed: int = 0) -> dict:
    arg_keys = jax.random.split(jax.random.key(seed), 23)
    mixer_microbatch = bell_draw(arg_keys[0], (TOKENS_A, D), 1.0, 6.0, ((0, 32),))
    mixer_gain_vector = jnp.clip(1.0 + 0.18 * jax.random.normal(arg_keys[1], (D,), jnp.float32), 0.1, 1.9)
    asker_matrix = bell_draw(arg_keys[2], (D, NUM_SUBSPACES * MATCHER_WIDTH), D ** -0.5, 0.125, ((1, 4),))
    matcher_matrix = bell_draw(arg_keys[3], (D, NUM_SUBSPACES * MATCHER_WIDTH), D ** -0.5, 0.125, ((1, 4),))
    fading_matrix = bell_draw(arg_keys[4], (D, NUM_SUBSPACES * MATCHER_WIDTH), D ** -0.5, 0.125, ((1, 4),))
    content_matrix = bell_draw(arg_keys[5], (D, NUM_SUBSPACES * DV), D ** -0.5, 0.125, ((1, 4),))
    result_valve_matrix = bell_draw(arg_keys[6], (D, NUM_SUBSPACES * DV), D ** -0.5, 0.125, ((1, 4),))
    fading_shift_vector = draw_fading_shift_vector(jax.random.fold_in(arg_keys[22], 71), 0)
    extra_fade_amount = draw_extra_fade_amount(jax.random.fold_in(arg_keys[22], 71), 0)
    starting_memory = bell_draw(arg_keys[9], (NUM_SUBSPACES * MATCHER_WIDTH, DV), 4.0, 24.0, ((0, 4),), jnp.float32)
    subspace_gain_vector = jnp.clip(1.0 + 0.18 * jax.random.normal(arg_keys[10], (NUM_SUBSPACES * DV,), jnp.float32), 0.1, 1.9)
    result_matrix = bell_draw(arg_keys[11], (NUM_SUBSPACES * DV, D), (NUM_SUBSPACES * DV) ** -0.5, 0.125)
    specialist_microbatch = bell_draw(arg_keys[12], (TOKENS_B, D), 1.0, 6.0, ((0, 32),))
    specialist_gain_vector = jnp.clip(1.0 + 0.18 * jax.random.normal(arg_keys[13], (D,), jnp.float32), 0.1, 1.9)
    picked_specialists_keys = jax.random.split(jax.random.fold_in(arg_keys[14], 1), TOKENS_B // TOK_MOE)
    picked_specialists_turns = jax.random.permutation(jax.random.fold_in(arg_keys[14], 3), TOKENS_B // TOK_MOE)
    picked_specialists = jax.vmap(lambda own, number: shared_out(jax.random.fold_in(arg_keys[14], 2), own, number, TOK_MOE, EXPERTS, TOP_K, CAP, 1))(picked_specialists_keys, picked_specialists_turns).reshape((TOKENS_B, TOP_K))
    specialist_mixing_factor = jnp.clip(jnp.exp(math.log(1.5) - 1.60943787 * jax.random.uniform(arg_keys[15], (TOKENS_B, TOP_K), jnp.float32) ** block_scale(arg_keys[15], (TOKENS_B, TOP_K), ((0, 32),), -0.2, 0.2)), 0.3, 1.5)
    specialist_valve_matrix = bell_draw(arg_keys[16], (EXPERTS, D, FFE), D ** -0.5, 0.125, ((0, 8), (2, 4)))
    specialist_widen_matrix = bell_draw(arg_keys[17], (EXPERTS, D, FFE), D ** -0.5, 0.125, ((0, 8), (2, 4)))
    specialist_shrink_matrix = bell_draw(arg_keys[18], (EXPERTS, FFE, D), FFE ** -0.5, 0.1875, ((0, 8), (1, 4)))
    joint_valve_matrix = bell_draw(arg_keys[19], (D, FFS), D ** -0.5, 0.125, ((1, 4),))
    joint_widen_matrix = bell_draw(arg_keys[20], (D, FFS), D ** -0.5, 0.125, ((1, 4),))
    joint_shrink_matrix = bell_draw(arg_keys[21], (FFS, D), FFS ** -0.5, 0.25, ((0, 4),))
    return dict(mixer_microbatch=mixer_microbatch, mixer_gain_vector=mixer_gain_vector, asker_matrix=asker_matrix, matcher_matrix=matcher_matrix, fading_matrix=fading_matrix, content_matrix=content_matrix, result_valve_matrix=result_valve_matrix, fading_shift_vector=fading_shift_vector, extra_fade_amount=extra_fade_amount, starting_memory=starting_memory, subspace_gain_vector=subspace_gain_vector, result_matrix=result_matrix, specialist_microbatch=specialist_microbatch, specialist_gain_vector=specialist_gain_vector, picked_specialists=picked_specialists, specialist_mixing_factor=specialist_mixing_factor, specialist_valve_matrix=specialist_valve_matrix, specialist_widen_matrix=specialist_widen_matrix, specialist_shrink_matrix=specialist_shrink_matrix, joint_valve_matrix=joint_valve_matrix, joint_widen_matrix=joint_widen_matrix, joint_shrink_matrix=joint_shrink_matrix)


NORM_EPS = 1e-06
GATE_SOFTNESS = 16.0
exact_precision = lax.Precision.HIGHEST

def rms_rows(values, gain):
    widened = values.astype(jnp.float32)
    inverse_rms = lax.rsqrt(lax.optimization_barrier(jnp.mean(widened * widened, axis=-1, keepdims=True)) + NORM_EPS)
    return (widened * inverse_rms * gain).astype(jnp.bfloat16)

def expert_apply(rows_in, gate_w, up_w, down_w):
    gate_value = jnp.dot(rows_in, gate_w, preferred_element_type=jnp.float32)
    up_value = jnp.dot(rows_in, up_w, preferred_element_type=jnp.float32)
    hidden = (jax.nn.silu(gate_value) * up_value).astype(jnp.bfloat16)
    group_width = down_w.shape[0] // N_TP
    combined = jnp.zeros((rows_in.shape[0], down_w.shape[1]), jnp.float32)
    for group_index in range(N_TP):
        row_lower = group_index * group_width
        partial_sum = jnp.dot(hidden[:, row_lower:row_lower + group_width], down_w[row_lower:row_lower + group_width], preferred_element_type=jnp.float32)
        rounded = lax.optimization_barrier(partial_sum.astype(jnp.bfloat16))
        combined = combined + rounded.astype(jnp.float32)
    return combined.astype(jnp.bfloat16)

def mixer_share(mixer_microbatch, mixer_gain_vector, asker_matrix, matcher_matrix, fading_matrix, content_matrix, result_valve_matrix, fading_shift_vector, extra_fade_amount, starting_memory, subspace_gain_vector, result_matrix):
    normed = rms_rows(mixer_microbatch, mixer_gain_vector)

    def project(weight):
        return jnp.dot(normed, weight, preferred_element_type=jnp.float32).astype(jnp.bfloat16)
    query, key_rows, decay_logits, value, gate_pre = (project(asker_matrix), project(matcher_matrix), project(fading_matrix), project(content_matrix), project(result_valve_matrix))
    logarithmic_fading_speed = jax.nn.log_sigmoid(decay_logits.astype(jnp.float32) + fading_shift_vector) / GATE_SOFTNESS
    span_sequence = TOKENS_A // SPAN_LENGTH
    dimension_signature = (span_sequence, SPAN_LENGTH, NUM_SUBSPACES, MATCHER_WIDTH)
    query_wide = query.astype(jnp.float32).reshape(dimension_signature) * MATCHER_WIDTH ** (-0.5)
    key_wide = key_rows.astype(jnp.float32).reshape(dimension_signature)
    value_wide = value.astype(jnp.float32).reshape(span_sequence, SPAN_LENGTH, NUM_SUBSPACES, DV)
    speed_expanded = logarithmic_fading_speed.reshape(dimension_signature) + extra_fade_amount.reshape(span_sequence, SPAN_LENGTH, NUM_SUBSPACES, 1)
    causal_mask = jnp.tril(jnp.ones((SPAN_LENGTH, SPAN_LENGTH), bool))

    def step(carried_state, inputs):
        query_block, key_block, block_values, rate_block = inputs
        running = jnp.cumsum(rate_block, axis=0)
        block_total = running[-1:]
        query_faded = query_block * jnp.exp(running)
        k_decayed = key_block * jnp.exp(-running)
        key_until_finish = key_block * jnp.exp(block_total - running)
        scores = jnp.einsum('ihk,jhk->hij', query_faded, k_decayed, precision=exact_precision)
        scores = jnp.where(causal_mask[None], scores, 0.0)
        inner_part = jnp.einsum('hij,jhv->ihv', scores, block_values, precision=exact_precision)
        outer_contribution = jnp.einsum('wzr,zrg->wzg', query_faded, carried_state, precision=exact_precision)
        added_terms = jnp.einsum('aqe,aqf->qef', key_until_finish, block_values, precision=exact_precision)
        updated = jnp.exp(block_total[0])[..., None] * carried_state + added_terms
        return (updated, inner_part + outer_contribution)
    first_state = starting_memory.astype(jnp.float32).reshape(NUM_SUBSPACES, MATCHER_WIDTH, DV)
    _, attended = lax.scan(step, first_state, (query_wide, key_wide, value_wide, speed_expanded))
    attended = attended.reshape(TOKENS_A, NUM_SUBSPACES, DV)
    inverse_rms = lax.rsqrt(lax.optimization_barrier(jnp.mean(attended * attended, axis=-1, keepdims=True)) + NORM_EPS)
    normed_heads = (attended * inverse_rms).reshape(TOKENS_A, NUM_SUBSPACES * DV) * subspace_gain_vector
    headed = (normed_heads * jax.nn.silu(gate_pre.astype(jnp.float32))).astype(jnp.bfloat16)
    return jnp.dot(headed, result_matrix, preferred_element_type=jnp.float32).astype(jnp.bfloat16)

def expert_half(specialist_microbatch, specialist_gain_vector, picked_specialists, specialist_mixing_factor, specialist_valve_matrix, specialist_widen_matrix, specialist_shrink_matrix, joint_valve_matrix, joint_widen_matrix, joint_shrink_matrix):
    normed = rms_rows(specialist_microbatch, specialist_gain_vector)
    devices = N_EP * N_TP
    flat_expert = picked_specialists.reshape(devices, TOK_MOE * TOP_K)
    matches = (flat_expert[..., None] == jnp.arange(EXPERTS, dtype=jnp.int32)).astype(jnp.int32)
    slot_rank = lax.optimization_barrier(jnp.sum(jnp.cumsum(matches, axis=1) * matches, axis=2)) - 1
    device_ids = jnp.arange(devices, dtype=jnp.int32)[:, None]
    column = device_ids * CAP + slot_rank
    token_ids = device_ids * TOK_MOE + jnp.arange(TOK_MOE * TOP_K, dtype=jnp.int32)[None, :] // TOP_K
    slot_table = jnp.full((EXPERTS, devices * CAP), TOKENS_B, jnp.int32).at[flat_expert, column].set(token_ids)
    padded = jnp.concatenate([normed, jnp.zeros((1, normed.shape[1]), jnp.bfloat16)], axis=0)

    def one_expert(expert_index):
        picked_rows = padded[slot_table[expert_index]]
        return expert_apply(picked_rows, specialist_valve_matrix[expert_index], specialist_widen_matrix[expert_index], specialist_shrink_matrix[expert_index])
    outputs = lax.map(one_expert, jnp.arange(EXPERTS, dtype=jnp.int32))
    picked = outputs[flat_expert, column].reshape(TOKENS_B, TOP_K, normed.shape[1])
    shared = expert_apply(normed, joint_valve_matrix, joint_widen_matrix, joint_shrink_matrix)
    combined = shared.astype(jnp.float32) + lax.optimization_barrier(jnp.sum(specialist_mixing_factor[:, :, None] * picked.astype(jnp.float32), axis=1))
    return combined.astype(jnp.bfloat16)

def reference(mixer_microbatch, mixer_gain_vector, asker_matrix, matcher_matrix, fading_matrix, content_matrix, result_valve_matrix, fading_shift_vector, extra_fade_amount, starting_memory, subspace_gain_vector, result_matrix, specialist_microbatch, specialist_gain_vector, picked_specialists, specialist_mixing_factor, specialist_valve_matrix, specialist_widen_matrix, specialist_shrink_matrix, joint_valve_matrix, joint_widen_matrix, joint_shrink_matrix):
    mixer_sublayer_result = mixer_share(mixer_microbatch, mixer_gain_vector, asker_matrix, matcher_matrix, fading_matrix, content_matrix, result_valve_matrix, fading_shift_vector, extra_fade_amount, starting_memory, subspace_gain_vector, result_matrix)
    moe_out = expert_half(specialist_microbatch, specialist_gain_vector, picked_specialists, specialist_mixing_factor, specialist_valve_matrix, specialist_widen_matrix, specialist_shrink_matrix, joint_valve_matrix, joint_widen_matrix, joint_shrink_matrix)
    return (mixer_sublayer_result, moe_out)
```

```python
import jax
import jax.numpy as jnp
from jax import lax
from jax.experimental import pallas as pl
from jax.experimental.pallas import tpu as pltpu
from jax.sharding import PartitionSpec as P

MATCHER_WIDTH = 64
DV = 128
SPAN_LENGTH = 64


NORM_EPS = 1e-06
GATE_SOFTNESS = 16.0

NT = (((1,), (1,)), ((), ()))
TN = (((0,), (0,)), ((), ()))


def rms_rows(values, gain):
    widened = values.astype(jnp.float32)
    inverse_rms = lax.rsqrt(jnp.mean(widened * widened, axis=-1, keepdims=True) + NORM_EPS)
    return (widened * inverse_rms * gain).astype(jnp.bfloat16)


def dot32(a, b, dims=None):
    if dims is None:
        return jnp.dot(a, b, preferred_element_type=jnp.float32)
    return lax.dot_general(a, b, dims, preferred_element_type=jnp.float32)


def local_kernel(q_ref, k_ref, f_ref, v_ref, shift_ref, extra_ref, att_ref, qd_ref, state_ref, total_ref):
    span = SPAN_LENGTH
    pair_lanes = 2 * MATCHER_WIDTH
    rows_i = lax.broadcasted_iota(jnp.int32, (span, span), 0)
    cols_i = lax.broadcasted_iota(jnp.int32, (span, span), 1)
    lower = rows_i >= cols_i
    summing = lower.astype(jnp.float32).astype(jnp.bfloat16)
    causal = jnp.concatenate([lower, lower], axis=0)
    first = lax.broadcasted_iota(jnp.int32, (1, pair_lanes), 1) < MATCHER_WIDTH
    shift = shift_ref[...]
    spans = q_ref.shape[0] // span
    unroll = 4 if spans % 4 == 0 else 1

    def one(n, carry):
        state, total = carry
        rows = pl.ds(pl.multiple_of(n * span, span), span)
        pre = f_ref[rows, :].astype(jnp.float32) + shift
        log_sig = jnp.minimum(pre, 0.0) - jnp.log1p(jnp.exp(-jnp.abs(pre)))
        rate = log_sig * (1.0 / GATE_SOFTNESS) + extra_ref[rows, :]
        high = rate.astype(jnp.bfloat16)
        low = (rate - high.astype(jnp.float32)).astype(jnp.bfloat16)
        running = dot32(summing, high) + dot32(summing, low)
        block_total = running[span - 1 :, :]
        faded = q_ref[rows, :].astype(jnp.float32) * jnp.exp(running) * MATCHER_WIDTH ** (-0.5)
        keys = k_ref[rows, :].astype(jnp.float32)
        k_decayed = (keys * jnp.exp(-running)).astype(jnp.bfloat16)
        k_finish = (keys * jnp.exp(block_total - running)).astype(jnp.bfloat16)
        both = jnp.concatenate(
            [jnp.where(first, faded, 0.0), jnp.where(first, 0.0, faded)], axis=0
        ).astype(jnp.bfloat16)
        scores = jnp.where(causal, dot32(both, k_decayed, NT), 0.0).astype(jnp.bfloat16)
        outer = dot32(both, state.astype(jnp.bfloat16), NT)
        value_a = v_ref[rows, :DV]
        value_b = v_ref[rows, DV:]
        att_ref[rows, :DV] = outer[:span] + dot32(scores[:span], value_a)
        att_ref[rows, DV:] = outer[span:] + dot32(scores[span:], value_b)
        added = jnp.where(first, dot32(value_a, k_finish, TN), dot32(value_b, k_finish, TN))
        qd_ref[rows, :] = (faded * jnp.exp(total)).astype(jnp.bfloat16)
        return (jnp.exp(block_total) * state + added, total + block_total)

    def group(g, carry):
        for u in range(unroll):
            carry = one(g * unroll + u, carry)
        return carry

    state, total = lax.fori_loop(
        0,
        spans // unroll,
        group,
        (jnp.zeros((DV, pair_lanes), jnp.float32), jnp.zeros((1, pair_lanes), jnp.float32)),
    )
    state_ref[...] = state.astype(jnp.bfloat16)[None]
    total_ref[...] = jnp.broadcast_to(jnp.exp(total), (1,) + total_ref.shape[1:]).astype(jnp.bfloat16)


def finish_kernel(att_ref, qd_ref, g_ref, gain_ref, enter_ref, out_ref):
    first = lax.broadcasted_iota(jnp.int32, (1, 2 * MATCHER_WIDTH), 1) < MATCHER_WIDTH
    enter = enter_ref[0].astype(jnp.bfloat16)
    qd = qd_ref[...].astype(jnp.float32)
    for half in range(2):
        own = jnp.where(first if half == 0 else jnp.logical_not(first), qd, 0.0).astype(jnp.bfloat16)
        cols = slice(half * DV, (half + 1) * DV)
        att = att_ref[:, cols] + dot32(own, enter, NT)
        inverse = lax.rsqrt(jnp.mean(att * att, axis=-1, keepdims=True) + NORM_EPS)
        gate = g_ref[:, cols].astype(jnp.float32)
        gated = att * inverse * gain_ref[:, cols] * (gate / (1.0 + jnp.exp(-gate)))
        out_ref[:, cols] = gated.astype(jnp.bfloat16)


def mixer_share(
    mixer_microbatch,
    mixer_gain_vector,
    asker_matrix,
    matcher_matrix,
    fading_matrix,
    content_matrix,
    result_valve_matrix,
    fading_shift_vector,
    extra_fade_amount,
    starting_memory,
    subspace_gain_vector,
    result_matrix,
):
    normed = rms_rows(mixer_microbatch, mixer_gain_vector)
    rows = lax.all_gather(normed, "tp", axis=0, tiled=True)
    number_tokens = rows.shape[0]
    value_width = content_matrix.shape[1]
    local_subspaces = value_width // DV
    pairs = local_subspaces // 2
    pair_lanes = 2 * MATCHER_WIDTH
    extra = jnp.repeat(extra_fade_amount, MATCHER_WIDTH, axis=1)

    def project(weight):
        return dot32(rows, weight).astype(jnp.bfloat16)

    query, keys, decay_pre, value, gate_pre = (
        project(asker_matrix),
        project(matcher_matrix),
        project(fading_matrix),
        project(content_matrix),
        project(result_valve_matrix),
    )
    narrow = pl.BlockSpec((number_tokens, pair_lanes), lambda p: (0, p))
    wide = pl.BlockSpec((number_tokens, 2 * DV), lambda p: (0, p))
    attended, query_far, local_end, device_fade = pl.pallas_call(
        local_kernel,
        grid=(pairs,),
        in_specs=[narrow, narrow, narrow, wide, pl.BlockSpec((1, pair_lanes), lambda p: (0, p)), narrow],
        out_specs=[
            wide,
            narrow,
            pl.BlockSpec((1, DV, pair_lanes), lambda p: (p, 0, 0)),
            pl.BlockSpec((1, 16, pair_lanes), lambda p: (p, 0, 0)),
        ],
        out_shape=[
            jax.ShapeDtypeStruct((number_tokens, value_width), jnp.float32),
            jax.ShapeDtypeStruct((number_tokens, pairs * pair_lanes), jnp.bfloat16),
            jax.ShapeDtypeStruct((pairs, DV, pair_lanes), jnp.bfloat16),
            jax.ShapeDtypeStruct((pairs, 16, pair_lanes), jnp.bfloat16),
        ],
        cost_estimate=pl.CostEstimate(flops=20_000_000_000, bytes_accessed=8_000_000, transcendentals=0),
        name="gla_local",
    )(query, keys, decay_pre, value, fading_shift_vector[None], extra)
    packed = jnp.concatenate([local_end, device_fade], axis=1)
    gathered = lax.all_gather(packed, "ep")
    place = lax.axis_index("ep")
    entering = starting_memory.reshape(pairs, pair_lanes, DV).transpose(0, 2, 1)
    for turn in range(gathered.shape[0]):
        part = gathered[turn].astype(jnp.float32)
        entering = jnp.where(
            turn < place, part[:, DV : DV + 1, :] * entering + part[:, :DV, :], entering
        )
    block = min(256, number_tokens)
    gated_rows = pl.pallas_call(
        finish_kernel,
        grid=(pairs, number_tokens // block),
        in_specs=[
            pl.BlockSpec((block, 2 * DV), lambda p, i: (i, p)),
            pl.BlockSpec((block, pair_lanes), lambda p, i: (i, p)),
            pl.BlockSpec((block, 2 * DV), lambda p, i: (i, p)),
            pl.BlockSpec((1, 2 * DV), lambda p, i: (0, p)),
            pl.BlockSpec((1, DV, pair_lanes), lambda p, i: (p, 0, 0)),
        ],
        out_specs=pl.BlockSpec((block, 2 * DV), lambda p, i: (i, p)),
        out_shape=jax.ShapeDtypeStruct((number_tokens, value_width), jnp.bfloat16),
        cost_estimate=pl.CostEstimate(flops=5_000_000_000, bytes_accessed=5_000_000, transcendentals=0),
        name="gla_finish",
    )(attended, query_far, gate_pre, subspace_gain_vector[None], entering)
    per_token = lax.all_to_all(gated_rows, "tp", split_axis=0, concat_axis=1, tiled=True)
    return dot32(per_token, result_matrix).astype(jnp.bfloat16)


def expert_half(
    specialist_microbatch,
    specialist_gain_vector,
    picked_specialists,
    specialist_mixing_factor,
    specialist_valve_matrix,
    specialist_widen_matrix,
    specialist_shrink_matrix,
    joint_valve_matrix,
    joint_widen_matrix,
    joint_shrink_matrix,
):
    ep_count = lax.axis_size("ep")
    me = lax.axis_index("ep")
    local_tokens, feature_width = specialist_microbatch.shape
    top_count = picked_specialists.shape[1]
    local_experts = specialist_widen_matrix.shape[0]
    experts = local_experts * ep_count
    slots = max(2, 3 * local_tokens * top_count // (2 * experts))
    expert_rows = ep_count * slots
    normed = rms_rows(specialist_microbatch, specialist_gain_vector)
    flat_expert = picked_specialists.reshape(-1)
    matches = flat_expert[:, None] == jnp.arange(experts, dtype=jnp.int32)[None, :]
    counts = jnp.arange(local_tokens * top_count, dtype=jnp.int32)
    earlier = (counts[:, None] > counts[None, :]).astype(jnp.bfloat16)
    before = dot32(earlier, matches.astype(jnp.bfloat16))
    rank = jnp.sum(jnp.where(matches, before, 0.0), axis=1).astype(jnp.int32)
    turn = lax.rem(flat_expert // local_experts - me + ep_count, ep_count)
    position = (lax.rem(flat_expert, local_experts) * ep_count + turn) * slots + rank
    position = position.reshape(local_tokens, top_count)
    places = jnp.arange(local_experts * expert_rows, dtype=jnp.int32)
    hits = position[:, :, None] == places[None, None, :]
    chosen = jnp.any(hits, axis=1).astype(jnp.bfloat16)
    outgoing = dot32(chosen, normed, TN).astype(jnp.bfloat16)
    outgoing = outgoing.reshape(local_experts, ep_count, slots, feature_width)

    def shared_part():
        rows = lax.all_gather(normed, "tp", axis=0, tiled=True)
        hidden = jax.nn.silu(dot32(rows, joint_valve_matrix)) * dot32(rows, joint_widen_matrix)
        partial = dot32(hidden.astype(jnp.bfloat16), joint_shrink_matrix).astype(jnp.bfloat16)
        return lax.psum_scatter(partial, "tp", scatter_dimension=0, tiled=True)

    def moved(blocks, sign):
        got = [blocks[0]]
        for step in range(1, ep_count):
            ring = [(i, (i + sign * step) % ep_count) for i in range(ep_count)]
            got.append(lax.ppermute(blocks[step], "ep", ring))
        return jnp.concatenate(got, axis=0)

    arrived = [moved(outgoing[e], 1) for e in range(local_experts)]
    shared = shared_part()
    tables = []
    for e in range(local_experts):
        rows = lax.all_gather(arrived[e], "tp", axis=0, tiled=True)
        gate_value = dot32(rows, specialist_valve_matrix[e])
        up_value = dot32(rows, specialist_widen_matrix[e])
        hidden = (jax.nn.silu(gate_value) * up_value).astype(jnp.bfloat16)
        partial = dot32(hidden, specialist_shrink_matrix[e]).astype(jnp.bfloat16)
        summed = lax.psum_scatter(partial, "tp", scatter_dimension=0, tiled=True)
        tables.append(moved(summed.reshape(ep_count, slots, feature_width), -1))
    weights = jnp.sum(jnp.where(hits, specialist_mixing_factor[:, :, None], 0.0), axis=1)
    high = weights.astype(jnp.bfloat16)
    low = (weights - high.astype(jnp.float32)).astype(jnp.bfloat16)
    combined = shared.astype(jnp.float32)
    for e in range(local_experts):
        part = slice(e * expert_rows, (e + 1) * expert_rows)
        combined = combined + dot32(high[:, part], tables[e]) + dot32(low[:, part], tables[e])
    return combined.astype(jnp.bfloat16)


def body(
    mixer_microbatch,
    mixer_gain_vector,
    asker_matrix,
    matcher_matrix,
    fading_matrix,
    content_matrix,
    result_valve_matrix,
    fading_shift_vector,
    extra_fade_amount,
    starting_memory,
    subspace_gain_vector,
    result_matrix,
    specialist_microbatch,
    specialist_gain_vector,
    picked_specialists,
    specialist_mixing_factor,
    specialist_valve_matrix,
    specialist_widen_matrix,
    specialist_shrink_matrix,
    joint_valve_matrix,
    joint_widen_matrix,
    joint_shrink_matrix,
):
    mixer_sublayer_result = mixer_share(
        mixer_microbatch,
        mixer_gain_vector,
        asker_matrix,
        matcher_matrix,
        fading_matrix,
        content_matrix,
        result_valve_matrix,
        fading_shift_vector,
        extra_fade_amount,
        starting_memory,
        subspace_gain_vector,
        result_matrix,
    )
    moe_out = expert_half(
        specialist_microbatch,
        specialist_gain_vector,
        picked_specialists,
        specialist_mixing_factor,
        specialist_valve_matrix,
        specialist_widen_matrix,
        specialist_shrink_matrix,
        joint_valve_matrix,
        joint_widen_matrix,
        joint_shrink_matrix,
    )
    return (mixer_sublayer_result, moe_out)


def solution(mesh):
    return jax.shard_map(
        body,
        mesh=mesh,
        in_specs=(
            P(("ep", "tp"), None),
            P(),
            P(None, "tp"),
            P(None, "tp"),
            P(None, "tp"),
            P(None, "tp"),
            P(None, "tp"),
            P("tp"),
            P("ep", "tp"),
            P("tp", None),
            P("tp"),
            P(),
            P(("ep", "tp"), None),
            P(),
            P(("ep", "tp"), None),
            P(("ep", "tp"), None),
            P("ep", None, "tp"),
            P("ep", None, "tp"),
            P("ep", "tp", None),
            P(None, "tp"),
            P(None, "tp"),
            P("tp", None),
        ),
        out_specs=(P(("ep", "tp"), None), P(("ep", "tp"), None)),
        check_vma=False,
    )
```

```python
import functools

import jax
import jax.numpy as jnp
from jax import lax
from jax.experimental import pallas as pl
from jax.experimental.pallas import tpu as pltpu
from jax.sharding import PartitionSpec as P

MATCHER_WIDTH = 64
DV = 128
SPAN_LENGTH = 64


NORM_EPS = 1e-06
GATE_SOFTNESS = 16.0

NT = (((1,), (1,)), ((), ()))
TN = (((0,), (0,)), ((), ()))


def rms_rows(values, gain):
    widened = values.astype(jnp.float32)
    inverse_rms = lax.rsqrt(jnp.mean(widened * widened, axis=-1, keepdims=True) + NORM_EPS)
    return (widened * inverse_rms * gain).astype(jnp.bfloat16)


def dot32(a, b, dims=None):
    if dims is None:
        return jnp.dot(a, b, preferred_element_type=jnp.float32)
    return lax.dot_general(a, b, dims, preferred_element_type=jnp.float32)


def local_kernel(q_ref, k_ref, f_ref, v_ref, shift_ref, extra_ref, att_ref, qd_ref, packed_ref):
    span = SPAN_LENGTH
    pair_lanes = 2 * MATCHER_WIDTH
    rows_i = lax.broadcasted_iota(jnp.int32, (span, span), 0)
    cols_i = lax.broadcasted_iota(jnp.int32, (span, span), 1)
    lower = rows_i >= cols_i
    summing = lower.astype(jnp.float32).astype(jnp.bfloat16)
    causal = jnp.concatenate([lower, lower], axis=0)
    first = lax.broadcasted_iota(jnp.int32, (1, pair_lanes), 1) < MATCHER_WIDTH
    shift = shift_ref[...]
    spans = q_ref.shape[0] // span
    unroll = 4 if spans % 4 == 0 else 1

    def one(n, carry):
        state, total = carry
        rows = pl.ds(pl.multiple_of(n * span, span), span)
        pre = f_ref[rows, :].astype(jnp.float32) + shift
        log_sig = jnp.minimum(pre, 0.0) - jnp.log1p(jnp.exp(-jnp.abs(pre)))
        rate = log_sig * (1.0 / GATE_SOFTNESS) + extra_ref[rows, :]
        high = rate.astype(jnp.bfloat16)
        low = (rate - high.astype(jnp.float32)).astype(jnp.bfloat16)
        running = dot32(summing, high) + dot32(summing, low)
        block_total = running[span - 1 :, :]
        faded = q_ref[rows, :].astype(jnp.float32) * jnp.exp(running) * MATCHER_WIDTH ** (-0.5)
        keys = k_ref[rows, :].astype(jnp.float32)
        k_decayed = (keys * jnp.exp(-running)).astype(jnp.bfloat16)
        k_finish = (keys * jnp.exp(block_total - running)).astype(jnp.bfloat16)
        both = jnp.concatenate(
            [jnp.where(first, faded, 0.0), jnp.where(first, 0.0, faded)], axis=0
        ).astype(jnp.bfloat16)
        scores = jnp.where(causal, dot32(both, k_decayed, NT), 0.0).astype(jnp.bfloat16)
        outer = dot32(both, state.astype(jnp.bfloat16), NT)
        value_a = v_ref[rows, :DV]
        value_b = v_ref[rows, DV:]
        att_ref[rows, :DV] = outer[:span] + dot32(scores[:span], value_a)
        att_ref[rows, DV:] = outer[span:] + dot32(scores[span:], value_b)
        added = jnp.where(first, dot32(value_a, k_finish, TN), dot32(value_b, k_finish, TN))
        qd_ref[rows, :] = (faded * jnp.exp(total)).astype(jnp.bfloat16)
        return (jnp.exp(block_total) * state + added, total + block_total)

    def group(g, carry):
        for u in range(unroll):
            carry = one(g * unroll + u, carry)
        return carry

    state, total = lax.fori_loop(
        0,
        spans // unroll,
        group,
        (jnp.zeros((DV, pair_lanes), jnp.float32), jnp.zeros((1, pair_lanes), jnp.float32)),
    )
    packed_ref[:, :DV, :] = state.astype(jnp.bfloat16)[None]
    packed_ref[:, DV:, :] = jnp.broadcast_to(jnp.exp(total), (1, 16, pair_lanes)).astype(jnp.bfloat16)


def finish_kernel(att_ref, qd_ref, g_ref, gain_ref, enter_ref, out_ref):
    first = lax.broadcasted_iota(jnp.int32, (1, 2 * MATCHER_WIDTH), 1) < MATCHER_WIDTH
    enter = enter_ref[0].astype(jnp.bfloat16)
    qd = qd_ref[...].astype(jnp.float32)
    for half in range(2):
        own = jnp.where(first if half == 0 else jnp.logical_not(first), qd, 0.0).astype(jnp.bfloat16)
        cols = slice(half * DV, (half + 1) * DV)
        att = att_ref[:, cols] + dot32(own, enter, NT)
        inverse = lax.rsqrt(jnp.mean(att * att, axis=-1, keepdims=True) + NORM_EPS)
        gate = g_ref[:, cols].astype(jnp.float32)
        gated = att * inverse * gain_ref[:, cols] * (gate / (1.0 + jnp.exp(-gate)))
        out_ref[:, cols] = gated.astype(jnp.bfloat16)


def exchange_kernel(ep_count, sign, lists, *refs):
    sources, landings = refs[:lists], refs[lists : 2 * lists]
    send_sem, recv_sem, own_sem = refs[2 * lists :]
    me = lax.axis_index("ep")
    barrier = pltpu.get_barrier_semaphore()
    for step in range(1, ep_count):
        peer = lax.rem(me + step, ep_count)
        pl.semaphore_signal(barrier, inc=1, device_id={"ep": peer}, device_id_type=pl.DeviceIdType.MESH)
    pl.semaphore_wait(barrier, ep_count - 1)
    copies = []
    for at in range(lists):
        for step in range(1, ep_count):
            copy = pltpu.make_async_remote_copy(
                src_ref=sources[at].at[step],
                dst_ref=landings[at].at[step],
                send_sem=send_sem.at[at, step],
                recv_sem=recv_sem.at[at, step],
                device_id={"ep": lax.rem(me + sign * step + ep_count, ep_count)},
                device_id_type=pl.DeviceIdType.MESH,
            )
            copy.start()
            copies.append(copy)
        own = pltpu.make_async_copy(sources[at].at[0], landings[at].at[0], own_sem.at[at])
        own.start()
        copies.append(own)
    for copy in copies:
        copy.wait()


def exchanged(blocks, ep_count, sign, identity):
    lists = len(blocks)
    return pl.pallas_call(
        functools.partial(exchange_kernel, ep_count, sign, lists),
        in_specs=[pl.BlockSpec(memory_space=pltpu.VMEM)] * lists,
        out_specs=[pl.BlockSpec(memory_space=pltpu.VMEM)] * lists,
        out_shape=[jax.ShapeDtypeStruct(b.shape, b.dtype) for b in blocks],
        scratch_shapes=[
            pltpu.SemaphoreType.DMA((lists, ep_count)),
            pltpu.SemaphoreType.DMA((lists, ep_count)),
            pltpu.SemaphoreType.DMA((lists,)),
        ],
        compiler_params=pltpu.CompilerParams(collective_id=identity, has_side_effects=True),
        cost_estimate=pl.CostEstimate(
            flops=15_000_000_000 * lists, bytes_accessed=2_000_000 * lists, transcendentals=0
        ),
        name=f"exchange_{identity}",
    )(*blocks)


def hidden_kernel(count, *refs):
    rows, (gate_ref, up_ref, down_ref), outs = refs[:count], refs[count : count + 3], refs[count + 3 :]
    for row_ref, out_ref in zip(rows, outs):
        gate = dot32(row_ref[...], gate_ref[0])
        hidden = gate / (1.0 + jnp.exp(-gate)) * dot32(row_ref[...], up_ref[0])
        out_ref[...] = dot32(hidden.astype(jnp.bfloat16), down_ref[0]).astype(jnp.bfloat16)


def hidden_part(blocks, gate_w, up_w, down_w, expert):
    count = len(blocks)
    rows, width = blocks[0].shape
    block_spec = pl.BlockSpec((rows, width), lambda i: (0, 0))
    weight = lambda w: pl.BlockSpec((1,) + w.shape[1:], lambda i: (expert, 0, 0))
    flops = 6 * count * rows * width * gate_w.shape[2]
    return pl.pallas_call(
        functools.partial(hidden_kernel, count),
        grid=(1,),
        in_specs=[block_spec] * count + [weight(gate_w), weight(up_w), weight(down_w)],
        out_specs=[block_spec] * count,
        out_shape=[jax.ShapeDtypeStruct((rows, width), jnp.bfloat16)] * count,
        cost_estimate=pl.CostEstimate(flops=2 * flops, bytes_accessed=8_000_000, transcendentals=0),
        name="hidden_part",
    )(*blocks, gate_w, up_w, down_w)


def spread_kernel(ep_count, own_ref, all_ref, send_sem, recv_sem, own_sem):
    me = lax.axis_index("ep")
    barrier = pltpu.get_barrier_semaphore()
    for step in range(1, ep_count):
        peer = lax.rem(me + step, ep_count)
        pl.semaphore_signal(barrier, inc=1, device_id={"ep": peer}, device_id_type=pl.DeviceIdType.MESH)
    pl.semaphore_wait(barrier, ep_count - 1)
    own = pltpu.make_async_copy(own_ref, all_ref.at[me], own_sem.at[0])
    own.start()
    copies = [own]
    for step in range(1, ep_count):
        copy = pltpu.make_async_remote_copy(
            src_ref=own_ref,
            dst_ref=all_ref.at[me],
            send_sem=send_sem.at[step],
            recv_sem=recv_sem.at[step],
            device_id={"ep": lax.rem(me + step, ep_count)},
            device_id_type=pl.DeviceIdType.MESH,
        )
        copy.start()
        copies.append(copy)
    for copy in copies:
        copy.wait()


def spread(own):
    ep_count = lax.axis_size("ep")
    return pl.pallas_call(
        functools.partial(spread_kernel, ep_count),
        in_specs=[pl.BlockSpec(memory_space=pltpu.VMEM)],
        out_specs=pl.BlockSpec(memory_space=pltpu.VMEM),
        out_shape=jax.ShapeDtypeStruct((ep_count,) + own.shape, own.dtype),
        scratch_shapes=[
            pltpu.SemaphoreType.DMA((ep_count,)),
            pltpu.SemaphoreType.DMA((ep_count,)),
            pltpu.SemaphoreType.DMA((1,)),
        ],
        compiler_params=pltpu.CompilerParams(collective_id=29, has_side_effects=True),
        cost_estimate=pl.CostEstimate(flops=12_000_000_000, bytes_accessed=1_000_000, transcendentals=0),
        name="spread",
    )(own)


def mixer_share(
    mixer_microbatch,
    mixer_gain_vector,
    asker_matrix,
    matcher_matrix,
    fading_matrix,
    content_matrix,
    result_valve_matrix,
    fading_shift_vector,
    extra_fade_amount,
    starting_memory,
    subspace_gain_vector,
    result_matrix,
):
    normed = rms_rows(mixer_microbatch, mixer_gain_vector)
    rows = lax.all_gather(normed, "tp", axis=0, tiled=True)
    number_tokens = rows.shape[0]
    value_width = content_matrix.shape[1]
    local_subspaces = value_width // DV
    pairs = local_subspaces // 2
    pair_lanes = 2 * MATCHER_WIDTH
    extra = jnp.repeat(extra_fade_amount, MATCHER_WIDTH, axis=1)

    def project(weight):
        return dot32(rows, weight).astype(jnp.bfloat16)

    query, keys, decay_pre, value, gate_pre = (
        project(asker_matrix),
        project(matcher_matrix),
        project(fading_matrix),
        project(content_matrix),
        project(result_valve_matrix),
    )
    narrow = pl.BlockSpec((number_tokens, pair_lanes), lambda p: (0, p))
    wide = pl.BlockSpec((number_tokens, 2 * DV), lambda p: (0, p))
    attended, query_far, packed = pl.pallas_call(
        local_kernel,
        grid=(pairs,),
        in_specs=[narrow, narrow, narrow, wide, pl.BlockSpec((1, pair_lanes), lambda p: (0, p)), narrow],
        out_specs=[
            wide,
            narrow,
            pl.BlockSpec((1, DV + 16, pair_lanes), lambda p: (p, 0, 0)),
        ],
        out_shape=[
            jax.ShapeDtypeStruct((number_tokens, value_width), jnp.float32),
            jax.ShapeDtypeStruct((number_tokens, pairs * pair_lanes), jnp.bfloat16),
            jax.ShapeDtypeStruct((pairs, DV + 16, pair_lanes), jnp.bfloat16),
        ],
        cost_estimate=pl.CostEstimate(flops=20_000_000_000, bytes_accessed=8_000_000, transcendentals=0),
        name="gla_local",
    )(query, keys, decay_pre, value, fading_shift_vector[None], extra)
    packed, gate_pre = lax.optimization_barrier((packed, gate_pre))
    ahead = yield packed
    packed, _ = lax.optimization_barrier((packed, ahead))
    gathered = spread(packed)
    yield gathered
    place = lax.axis_index("ep")
    entering = starting_memory.reshape(pairs, pair_lanes, DV).transpose(0, 2, 1)
    for turn in range(gathered.shape[0]):
        part = gathered[turn].astype(jnp.float32)
        entering = jnp.where(
            turn < place, part[:, DV : DV + 1, :] * entering + part[:, :DV, :], entering
        )
    block = min(256, number_tokens)
    gated_rows = pl.pallas_call(
        finish_kernel,
        grid=(pairs, number_tokens // block),
        in_specs=[
            pl.BlockSpec((block, 2 * DV), lambda p, i: (i, p)),
            pl.BlockSpec((block, pair_lanes), lambda p, i: (i, p)),
            pl.BlockSpec((block, 2 * DV), lambda p, i: (i, p)),
            pl.BlockSpec((1, 2 * DV), lambda p, i: (0, p)),
            pl.BlockSpec((1, DV, pair_lanes), lambda p, i: (p, 0, 0)),
        ],
        out_specs=pl.BlockSpec((block, 2 * DV), lambda p, i: (i, p)),
        out_shape=jax.ShapeDtypeStruct((number_tokens, value_width), jnp.bfloat16),
        cost_estimate=pl.CostEstimate(flops=5_000_000_000, bytes_accessed=5_000_000, transcendentals=0),
        name="gla_finish",
    )(attended, query_far, gate_pre, subspace_gain_vector[None], entering)
    yield gated_rows
    per_token = lax.all_to_all(gated_rows, "tp", split_axis=0, concat_axis=1, tiled=True)
    yield dot32(per_token, result_matrix).astype(jnp.bfloat16)


def expert_half(
    specialist_microbatch,
    specialist_gain_vector,
    picked_specialists,
    specialist_mixing_factor,
    specialist_valve_matrix,
    specialist_widen_matrix,
    specialist_shrink_matrix,
    joint_valve_matrix,
    joint_widen_matrix,
    joint_shrink_matrix,
    packed,
    mixer,
):
    ep_count = lax.axis_size("ep")
    tp_count = lax.axis_size("tp")
    me = lax.axis_index("ep")
    local_tokens, feature_width = specialist_microbatch.shape
    top_count = picked_specialists.shape[1]
    local_experts = specialist_widen_matrix.shape[0]
    experts = local_experts * ep_count
    slots = max(2, 3 * local_tokens * top_count // (2 * experts))
    expert_rows = ep_count * slots
    normed = rms_rows(specialist_microbatch, specialist_gain_vector)
    flat_expert = picked_specialists.reshape(-1)
    matches = flat_expert[:, None] == jnp.arange(experts, dtype=jnp.int32)[None, :]
    counts = jnp.arange(local_tokens * top_count, dtype=jnp.int32)
    earlier = (counts[:, None] > counts[None, :]).astype(jnp.bfloat16)
    before = dot32(earlier, matches.astype(jnp.bfloat16))
    rank = jnp.sum(jnp.where(matches, before, 0.0), axis=1).astype(jnp.int32)
    turn = lax.rem(flat_expert // local_experts - me + ep_count, ep_count)
    position = (lax.rem(flat_expert, local_experts) * ep_count + turn) * slots + rank
    position = position.reshape(local_tokens, top_count)
    places = jnp.arange(local_experts * expert_rows, dtype=jnp.int32)
    hits = position[:, :, None] == places[None, None, :]
    chosen = jnp.any(hits, axis=1).astype(jnp.bfloat16)
    outgoing = dot32(chosen, normed, TN).astype(jnp.bfloat16)
    outgoing = outgoing.reshape(local_experts, ep_count, slots, feature_width)

    def swapped(block, bit):
        return lax.ppermute(block, "tp", [(i, i ^ bit) for i in range(tp_count)])

    far = tp_count // 2

    def over_far(own):
        return {0: own, far: swapped(own, far)} if far else {0: own}

    def through(blocks, gate_w, up_w, down_w, expert):
        names = list(blocks)
        *held, _ = lax.optimization_barrier((*[blocks[r] for r in names], packed))
        blocks = dict(zip(names, held))
        bit = far // 2
        while bit:
            for r in list(blocks):
                blocks[r ^ bit] = swapped(blocks[r], bit)
            bit //= 2
        names = list(blocks)
        outs = hidden_part([blocks[r] for r in names], gate_w, up_w, down_w, expert)
        return summed_over(dict(zip(names, outs)), 1, far)

    def summed_over(parts, bit, stop, after=None):
        while bit < stop:
            joined = {}
            for r in parts:
                if not r & bit:
                    other = swapped(parts[r | bit], bit)
                    if after is not None:
                        other, _ = lax.optimization_barrier((other, after))
                    other = other.astype(jnp.float32)
                    joined[r] = (parts[r].astype(jnp.float32) + other).astype(jnp.bfloat16)
            parts = joined
            bit *= 2
        return parts

    arrived = []
    for e in range(local_experts):
        leaving = outgoing[e]
        if e:
            leaving, _ = lax.optimization_barrier((leaving, arrived[-1]))
        arrived += exchanged([leaving], ep_count, 1, e)
    shared_blocks = over_far(normed)
    blocks = [over_far(a.reshape(expert_rows, feature_width)) for a in arrived]
    parts = [
        through(
            blocks[e],
            specialist_valve_matrix,
            specialist_widen_matrix,
            specialist_shrink_matrix,
            e,
        )
        for e in range(local_experts)
    ]
    shared_parts = through(
        shared_blocks, joint_valve_matrix[None], joint_widen_matrix[None], joint_shrink_matrix[None], 0
    )
    gathered = mixer.send(parts[-1][0])
    summed = [summed_over(p, max(far, 1), tp_count, gathered)[0] for p in parts]
    shared = summed_over(shared_parts, max(far, 1), tp_count, gathered)[0]
    gated_rows = next(mixer)
    tables = []
    for e in range(local_experts):
        after = tables[-1] if e else gathered
        leaving = summed[e].reshape(ep_count, slots, feature_width)
        leaving, *_ = lax.optimization_barrier((leaving, after) + ((gated_rows,) if e else ()))
        (back,) = exchanged([leaving], ep_count, -1, local_experts + e)
        tables.append(back.reshape(expert_rows, feature_width))
    weights = jnp.sum(jnp.where(hits, specialist_mixing_factor[:, :, None], 0.0), axis=1)
    high = weights.astype(jnp.bfloat16)
    low = (weights - high.astype(jnp.float32)).astype(jnp.bfloat16)
    combined = shared.astype(jnp.float32)
    for e in range(local_experts):
        part = slice(e * expert_rows, (e + 1) * expert_rows)
        combined = combined + dot32(high[:, part], tables[e]) + dot32(low[:, part], tables[e])
    return combined.astype(jnp.bfloat16)


def body(
    mixer_microbatch,
    mixer_gain_vector,
    asker_matrix,
    matcher_matrix,
    fading_matrix,
    content_matrix,
    result_valve_matrix,
    fading_shift_vector,
    extra_fade_amount,
    starting_memory,
    subspace_gain_vector,
    result_matrix,
    specialist_microbatch,
    specialist_gain_vector,
    picked_specialists,
    specialist_mixing_factor,
    specialist_valve_matrix,
    specialist_widen_matrix,
    specialist_shrink_matrix,
    joint_valve_matrix,
    joint_widen_matrix,
    joint_shrink_matrix,
):
    mixer = mixer_share(
        mixer_microbatch,
        mixer_gain_vector,
        asker_matrix,
        matcher_matrix,
        fading_matrix,
        content_matrix,
        result_valve_matrix,
        fading_shift_vector,
        extra_fade_amount,
        starting_memory,
        subspace_gain_vector,
        result_matrix,
    )
    packed = next(mixer)
    moe_out = expert_half(
        specialist_microbatch,
        specialist_gain_vector,
        picked_specialists,
        specialist_mixing_factor,
        specialist_valve_matrix,
        specialist_widen_matrix,
        specialist_shrink_matrix,
        joint_valve_matrix,
        joint_widen_matrix,
        joint_shrink_matrix,
        packed,
        mixer,
    )
    mixer_sublayer_result = next(mixer)
    return (mixer_sublayer_result, moe_out)


def solution(mesh):
    return jax.shard_map(
        body,
        mesh=mesh,
        in_specs=(
            P(("ep", "tp"), None),
            P(),
            P(None, "tp"),
            P(None, "tp"),
            P(None, "tp"),
            P(None, "tp"),
            P(None, "tp"),
            P("tp"),
            P("ep", "tp"),
            P("tp", None),
            P("tp"),
            P(),
            P(("ep", "tp"), None),
            P(),
            P(("ep", "tp"), None),
            P(("ep", "tp"), None),
            P("ep", None, "tp"),
            P("ep", None, "tp"),
            P("ep", "tp", None),
            P(None, "tp"),
            P(None, "tp"),
            P("tp", None),
        ),
        out_specs=(P(("ep", "tp"), None), P(("ep", "tp"), None)),
        check_vma=False,
    )
```
